32 devices in a mesh: ep: 8 (over z, x), tp: 4 (over y, core).
Axes of the slice: x: 2, y: 2, z: 4, core: 2. Of those that a mesh axis runs over, the one named last changes fastest.
Arguments:
- resid: bfloat16 [256, 2048], P('ep'), may hold values from -6 to 6
- norm_gain: bfloat16 [2048], replicated, may hold values from 0.099609375 to 1.8984375
- w_query: bfloat16 [2048, 1024], P(None, 'tp'), may hold values from -0.125 to 0.125
- w_key: bfloat16 [2048, 1024], P(None, 'tp'), may hold values from -0.125 to 0.125
- w_value: bfloat16 [2048, 1024], P(None, 'tp'), may hold values from -0.125 to 0.125
- w_gate: bfloat16 [2048, 1024], P(None, 'tp'), may hold values from -0.125 to 0.125
- head_gain: bfloat16 [1024], P('tp'), may hold values from 0.099609375 to 1.8984375
- w_output: bfloat16 [1024, 2048], P('tp'), may hold values from -0.1875 to 0.1875
- state: float32 [256, 8, 128, 128], P('ep', 'tp'), may hold values from -0.6 to 0.6
- positions: int32 [256], P('ep'), may hold values from 1024 to 8191
- ffn_gain: bfloat16 [2048], replicated, may hold values from 0.099609375 to 1.8984375
- w_mix: bfloat16 [2048], replicated, may hold values from -0.125 to 0.125
- dense_gate: bfloat16 [2048, 5632], P('tp', 'ep'), may hold values from -0.125 to 0.125
- dense_up: bfloat16 [2048, 5632], P('tp', 'ep'), may hold values from -0.125 to 0.125
- dense_down: bfloat16 [5632, 2048], P('ep', 'tp'), may hold values from -0.109375 to 0.109375
- routes: int32 [256, 2], P('ep'), may hold values from 0 to 7, all different within a row; in each aligned block of 32 rows (0 to 31, 32 to 63, ...) at most 16 rows name the same one
- route_weight: bfloat16 [256, 2], P('ep'), may hold values from 0.19921875 to 1
- expert_gate: bfloat16 [8, 2048, 4096], P('ep', None, 'tp'), may hold values from -0.125 to 0.125
- expert_up: bfloat16 [8, 2048, 4096], P('ep', None, 'tp'), may hold values from -0.125 to 0.125
- expert_down: bfloat16 [8, 4096, 2048], P('ep', 'tp'), may hold values from -0.09375 to 0.09375
Outputs:
- final: bfloat16 [256, 2048], P('ep', 'tp')
- new_state: float32 [256, 8, 128, 128], P('ep', 'tp')
The draws below stay inside these ranges and needn't reach their ends.
Inputs may be any that keep to these rules, and one draw needn't show every extreme that they name: `routes`: each row names 2 different experts; in the rows of one index of ep no expert is named by more than 16 rows, a bound that some block reaches; every expert is named by some row.
All inputs are finite; a program needn't handle non-finite values.
Results may differ from the reference program's by a relative error of at most 0.018.
Values may be sent and summed in bfloat16 or wider, within the bound.
A program may use at most 64 MiB of HBM per device.

```python
import math
import jax
import jax.numpy as jnp
import numpy as np
from jax import lax

D = 2048
RET_HEADS = 8
HEAD_DIM = 128
RET_W = 1024
FFD = 5632
FFE = 4096
TOPK = 2
SEQ_DEV = 32
SEQS = 256
EXPERTS = 8
CAP = 16
N_EP = 8
N_TP = 4


def place_ends(values, key, low, top_value):
    place = [jax.random.randint(jax.random.fold_in(key, axis), (), 0, length) for axis, length in enumerate(values.shape)]
    longest = values.shape.index(max(values.shape))
    neighbour = place[:longest] + [(place[longest] + 1) % values.shape[longest]] + place[longest + 1:]
    return values.at[tuple(place)].set(low).at[tuple(neighbour)].set(top_value)


def with_spikes(entries, own_key, source, target, parts, factor):
    def block_of(axis_at):
        return (jnp.arange(entries.shape[axis_at]) // (entries.shape[axis_at] // parts)).reshape((-1,) + (1,) * (entries.ndim - 1 - axis_at))

    near = jax.random.permutation(own_key, parts)[block_of(target)]
    far = (block_of(target) + parts // 2) % parts
    return jnp.where((block_of(source) == near) | (block_of(source) == far), factor * entries, entries)


def level_of(rng, dims, shards, low, top_value):
    factor_of = 1.0
    for dim, parts in shards:
        draws = jax.random.uniform(jax.random.fold_in(jax.random.fold_in(rng, 6), dim), (parts,), jnp.float32, low / len(shards), top_value / len(shards))
        factor_of = factor_of * jnp.repeat(jnp.exp(draws), dims[dim] // parts).reshape((-1,) + (1,) * (len(dims) - 1 - dim))
    return factor_of


def shared_out(rng, own, number, rows, count, top, bound, lean):
    sequence = jax.random.permutation(rng, count)
    heavy_load, usual = load_shares(count, rows * top, bound, lean, True), load_shares(count, rows * top, bound, lean, False)
    places = jnp.arange(count)

    def named(tallies, offset_by):
        used = int((tallies > 0).sum())
        fixed = max(1, used // 4)
        moved = fixed + (places - fixed + offset_by * (used - fixed)) % max(1, count - fixed)
        return jnp.zeros((count,), jnp.int32).at[sequence[jnp.where(places < fixed, places, moved)]].set(jnp.asarray(tallies, jnp.int32))

    tallies = jnp.where(number % 4 == 0, named(heavy_load, number // 4), named(usual, number - number // 4 - 1))
    mixed = jax.random.permutation(jax.random.fold_in(own, 3), count)
    source_of, receiver = mixed[0:count // 2 * 2:2], mixed[1:count // 2 * 2:2]
    margin = jnp.minimum(tallies[source_of] - 1, bound - tallies[receiver]) // 2
    margin = jnp.where((source_of == sequence[0]) | (receiver == sequence[0]) | (tallies[receiver] == 0), 0, jnp.maximum(margin, 0))
    moved = jax.random.randint(jax.random.fold_in(own, 4), (count // 2,), 0, 1 << 20) % (margin + 1)
    tallies = tallies.at[source_of].add(-moved).at[receiver].add(moved)
    labels = jnp.searchsorted(jnp.cumsum(tallies), jnp.arange(rows * top), side="right").astype(jnp.int32)
    grid = labels.reshape(top, rows).T
    grid = grid[jax.random.permutation(jax.random.fold_in(own, 1), rows)]
    offset_by = jax.random.randint(jax.random.fold_in(own, 2), (rows, 1), 0, top)
    return jnp.take_along_axis(grid, (jnp.arange(top)[None, :] + offset_by) % top, axis=1)


def load_shares(number_of, total, limit, skew, full):
    portions = [(1 << 20) // math.isqrt(rank ** skew) + 1 for rank in range(1, number_of + 1)]
    largest = limit if full else min(limit, max(-(-total // number_of), total * portions[0] // sum(portions)))
    least = 1 if total - largest >= number_of - 1 else 0
    given, rest = [largest] + [least] * (number_of - 1), total - largest - least * (number_of - 1)
    while rest > 0:
        free = [i for i in range(1, number_of) if given[i] < largest] or [i for i in range(1, number_of) if given[i] < limit]
        mass, remaining = sum([portions[i] for i in free]), rest
        for i in free:
            extra = min(limit - given[i], max(1, remaining * portions[i] // mass), rest)
            given[i] = given[i] + extra
            rest = rest - extra
    return np.array(given)


def scatter_about(stream_key, dims, deviation, limit, cuts=(), held_as=jnp.bfloat16):
    values = jax.random.normal(stream_key, dims, jnp.float32) * deviation
    if len(cuts) > 0:
        values = level_of(stream_key, dims, cuts, -0.22, 0.18) * values
    return jnp.clip(values, min=-limit, max=limit).astype(held_as)


def heavy_noise(own_key, dims, scale, most, cuts, heavy, kind=jnp.bfloat16):
    values = scale * jax.random.normal(own_key, dims, jnp.float32)
    if cuts:
        values = values * level_of(own_key, dims, cuts, -0.22, 0.18)
    return jnp.clip(with_spikes(values, jax.random.fold_in(own_key, 3), *heavy), -most, most).astype(kind)


def setup_inputs(seed: int = 0) -> dict:
    splits = jax.random.split(jax.random.key(seed), 21)
    resid = scatter_about(splits[0], (SEQS, D), 1.0, 6.0, ((0, 8),))
    norm_gain = jnp.clip(1.0 + 0.18 * jax.random.normal(splits[1], (D,), jnp.float32), 0.099609375, 1.8984375).astype(jnp.bfloat16)
    w_query = scatter_about(splits[2], (D, RET_W), D ** -0.5, 0.125, ((1, 4),))
    w_key = scatter_about(splits[3], (D, RET_W), D ** -0.5, 0.125, ((1, 4),))
    w_value = scatter_about(splits[4], (D, RET_W), D ** -0.5, 0.125, ((1, 4),))
    w_gate = scatter_about(splits[5], (D, RET_W), D ** -0.5, 0.125, ((1, 4),))
    head_gain = jnp.clip(1.0 + 0.18 * jax.random.normal(splits[6], (RET_W,), jnp.float32), 0.099609375, 1.8984375).astype(jnp.bfloat16)
    w_output = scatter_about(splits[7], (RET_W, D), RET_W ** -0.5, 0.1875, ((0, 4),))
    state = scatter_about(splits[8], (SEQS, RET_HEADS, HEAD_DIM, HEAD_DIM), 0.1, 0.6, ((0, 8), (1, 4)), jnp.float32)
    positions = place_ends(jax.random.randint(splits[9], (SEQS,), 1024, 8192), jax.random.fold_in(splits[9], 1), 1024, 8191).astype(jnp.int32)
    ffn_gain = jnp.clip(1.0 + 0.18 * jax.random.normal(splits[10], (D,), jnp.float32), 0.099609375, 1.8984375).astype(jnp.bfloat16)
    w_mix = scatter_about(splits[11], (D,), D ** -0.5, 0.125)
    dense_gate = scatter_about(splits[12], (D, FFD), D ** -0.5, 0.125, ((0, 4), (1, 8)))
    dense_up = scatter_about(splits[13], (D, FFD), D ** -0.5, 0.125, ((0, 4), (1, 8)))
    dense_down = heavy_noise(splits[14], (FFD, D), FFD ** -0.5, 0.109375, ((0, 8), (1, 4)), (0, 1, 8, 2.0))
    routes_keys = jax.random.split(jax.random.fold_in(splits[15], 1), SEQS // SEQ_DEV)
    routes_turns = jax.random.permutation(jax.random.fold_in(splits[15], 3), SEQS // SEQ_DEV)
    routes = jax.vmap(lambda own, number: shared_out(jax.random.fold_in(splits[15], 2), own, number, SEQ_DEV, EXPERTS, TOPK, CAP, 2))(routes_keys, routes_turns).reshape((SEQS, TOPK))
    route_weight = jnp.clip(0.19921875 + 0.80078125 * jax.random.uniform(splits[16], (SEQS, TOPK), jnp.float32) ** level_of(splits[16], (SEQS, TOPK), ((0, 8),), -0.2, 0.2), 0.19921875, 1.0).astype(jnp.bfloat16)
    expert_gate = scatter_about(splits[17], (EXPERTS, D, FFE), D ** -0.5, 0.125, ((0, 8), (2, 4)))
    expert_up = scatter_about(splits[18], (EXPERTS, D, FFE), D ** -0.5, 0.125, ((0, 8), (2, 4)))
    expert_down = scatter_about(splits[19], (EXPERTS, FFE, D), FFE ** -0.5, 0.09375, ((0, 8), (1, 4)))
    return dict(resid=resid, norm_gain=norm_gain, w_query=w_query, w_key=w_key, w_value=w_value, w_gate=w_gate, head_gain=head_gain, w_output=w_output, state=state, positions=positions, ffn_gain=ffn_gain, w_mix=w_mix, dense_gate=dense_gate, dense_up=dense_up, dense_down=dense_down, routes=routes, route_weight=route_weight, expert_gate=expert_gate, expert_up=expert_up, expert_down=expert_down)


EPSILON = 1e-06
THETA = 10000.0

def rms_norm(inputs, scaling):
    square = lax.optimization_barrier(jnp.mean(inputs * inputs, axis=-1, keepdims=True))
    return inputs * lax.rsqrt(square + EPSILON) * scaling.astype(jnp.float32)

def rounded(partial_value):
    return lax.optimization_barrier(partial_value.astype(jnp.bfloat16)).astype(jnp.float32)

def rotate(inputs, places):
    halfway = inputs.shape[-1] // 2
    inverse = THETA ** (-jnp.arange(halfway, dtype=jnp.float32) / halfway)
    angles = places.astype(jnp.float32)[:, None] * inverse[None, :]
    cosine = jnp.cos(angles)[:, None, :]
    sine_of = jnp.sin(angles)[:, None, :]
    former = inputs[..., :halfway]
    latter = inputs[..., halfway:]
    return jnp.concatenate([former * cosine - latter * sine_of, former * sine_of + latter * cosine], axis=-1)

def retain(queries, keys_in, values_in, gating, memory, places, head_first, head_gain):
    seqs_here = queries.shape[0]
    heads_here = memory.shape[1]
    head_size = memory.shape[2]
    head_shape = (seqs_here, heads_here, head_size)
    query_rot = rotate(queries.astype(jnp.float32).reshape(head_shape), places)
    key_rot = rotate(keys_in.astype(jnp.float32).reshape(head_shape), places) * head_size ** (-0.5)
    value_heads = values_in.astype(jnp.float32).reshape(head_shape)
    head_index = head_first + jnp.arange(heads_here, dtype=jnp.float32)
    decays = 1.0 - jnp.exp2(-1.0 - 1.5 * head_index)
    within = lax.optimization_barrier(jnp.sum(query_rot * key_rot, axis=-1, keepdims=True)) * value_heads
    carried = jnp.einsum('shd,shde->she', query_rot, memory, precision=lax.Precision.HIGHEST) * decays[None, :, None]
    mixture = within + carried
    new_memory = decays[None, :, None, None] * memory + key_rot[:, :, :, None] * value_heads[:, :, None, :]
    centre = lax.optimization_barrier(jnp.mean(mixture, axis=-1, keepdims=True))
    spread = lax.optimization_barrier(jnp.mean(jnp.square(mixture - centre), axis=-1, keepdims=True))
    normed = ((mixture - centre) * lax.rsqrt(spread + EPSILON)).reshape(seqs_here, heads_here * head_size)
    normed = normed * head_gain.astype(jnp.float32)
    output = (jax.nn.silu(gating.astype(jnp.float32)) * normed).astype(jnp.bfloat16)
    return (output, new_memory)

def select_slots(route_ids, expert, max_rows):
    flat_ids = route_ids.reshape(-1)
    hits = (flat_ids == expert).astype(jnp.int32)
    ranks = jnp.cumsum(hits) - 1
    slot_range = jnp.arange(max_rows, dtype=jnp.int32)
    matches = (hits[None, :] == 1) & (ranks[None, :] == slot_range[:, None])
    flat_index = jnp.arange(flat_ids.shape[0], dtype=jnp.int32)
    picked = lax.optimization_barrier(jnp.sum(jnp.where(matches, flat_index[None, :], 0), axis=1)).astype(jnp.int32)
    filled = jnp.any(matches, axis=1)
    return (picked, filled)

def expert_hidden(chosen, gate_weight, up_weight):
    gate_value = jnp.dot(chosen, gate_weight, preferred_element_type=jnp.float32)
    up_value = jnp.dot(chosen, up_weight, preferred_element_type=jnp.float32)
    return (jax.nn.silu(gate_value) * up_value).astype(jnp.bfloat16)

def reference(resid, norm_gain, w_query, w_key, w_value, w_gate, head_gain, w_output, state, positions, ffn_gain, w_mix, dense_gate, dense_up, dense_down, routes, route_weight, expert_gate, expert_up, expert_down):
    normed_in = rms_norm(resid.astype(jnp.float32), norm_gain).astype(jnp.bfloat16)

    def project(weight):
        return jnp.dot(normed_in, weight, preferred_element_type=jnp.float32).astype(jnp.bfloat16)
    retained, new_state = retain(project(w_query), project(w_key), project(w_value), project(w_gate), state, positions, 0.0, head_gain)
    width_tp = w_output.shape[0] // N_TP
    attention = jnp.zeros(resid.shape, jnp.float32)
    for block in range(N_TP):
        lower = block * width_tp
        attention = attention + rounded(jnp.dot(retained[:, lower:lower + width_tp], w_output[lower:lower + width_tp], preferred_element_type=jnp.float32))
    middle = resid.astype(jnp.float32) + attention
    normed_mid = rms_norm(middle, ffn_gain).astype(jnp.bfloat16)
    mixing = jax.nn.sigmoid(jnp.dot(normed_mid, w_mix[:, None], preferred_element_type=jnp.float32))
    model_tp = D // N_TP
    gate_sum = jnp.zeros((resid.shape[0], FFD), jnp.float32)
    up_sum = jnp.zeros((resid.shape[0], FFD), jnp.float32)
    for block in range(N_TP):
        lower = block * model_tp
        columns = normed_mid[:, lower:lower + model_tp]
        gate_sum = gate_sum + rounded(jnp.dot(columns, dense_gate[lower:lower + model_tp], preferred_element_type=jnp.float32))
        up_sum = up_sum + rounded(jnp.dot(columns, dense_up[lower:lower + model_tp], preferred_element_type=jnp.float32))
    dense_hidden = (jax.nn.silu(gate_sum) * up_sum).astype(jnp.bfloat16)
    hidden_ep = FFD // N_EP

    def dense_block(total, block):
        lower = block * hidden_ep
        part_hidden = lax.dynamic_slice_in_dim(dense_hidden, lower, hidden_ep, 1)
        part_down = lax.dynamic_slice_in_dim(dense_down, lower, hidden_ep, 0)
        return (total + rounded(jnp.dot(part_hidden, part_down, preferred_element_type=jnp.float32)), None)
    dense_out, _ = lax.scan(dense_block, jnp.zeros(resid.shape, jnp.float32), jnp.arange(N_EP, dtype=jnp.int32))
    max_rows = N_EP * CAP
    expert_tp = FFE // N_TP
    flat_weight = route_weight.reshape(-1).astype(jnp.float32)

    def one_expert(total, expert):
        picked, filled = select_slots(routes, expert, max_rows)
        token_rows = picked // TOPK
        chosen = normed_mid[token_rows]
        hidden_e = expert_hidden(chosen, expert_gate[expert], expert_up[expert])
        summed = jnp.zeros((max_rows, D), jnp.float32)
        for block in range(N_TP):
            lower = block * expert_tp
            summed = summed + rounded(jnp.dot(hidden_e[:, lower:lower + expert_tp], expert_down[expert, lower:lower + expert_tp], preferred_element_type=jnp.float32))
        result = rounded(summed)
        weights_e = jnp.where(filled, flat_weight[picked], 0.0)
        total = total.at[token_rows].add(weights_e[:, None] * result)
        return (total, None)
    moe_out, _ = lax.scan(one_expert, jnp.zeros(resid.shape, jnp.float32), jnp.arange(EXPERTS, dtype=jnp.int32))
    final = (middle + moe_out + mixing * dense_out).astype(jnp.bfloat16)
    return (final, new_state)
```

```python
import functools

import jax
import jax.numpy as jnp
from jax import lax
from jax.experimental import pallas as pl
from jax.experimental.pallas import tpu as pltpu
from jax.sharding import PartitionSpec as P

EPSILON = 1e-06
THETA = 10000.0


def rms_norm(inputs, scaling):
    square = jnp.mean(inputs * inputs, axis=-1, keepdims=True)
    return inputs * lax.rsqrt(square + EPSILON) * scaling.astype(jnp.float32)


def rotate(inputs, places):
    halfway = inputs.shape[-1] // 2
    inverse = THETA ** (-jnp.arange(halfway, dtype=jnp.float32) / halfway)
    angles = places.astype(jnp.float32)[:, None] * inverse[None, :]
    cosine = jnp.cos(angles)[:, None, :]
    sine_of = jnp.sin(angles)[:, None, :]
    former = inputs[..., :halfway]
    latter = inputs[..., halfway:]
    return jnp.concatenate(
        [former * cosine - latter * sine_of, former * sine_of + latter * cosine], axis=-1
    )


def retain(queries, keys_in, values_in, gating, memory, places, head_first, head_gain):
    seqs_here = queries.shape[0]
    heads_here = memory.shape[1]
    head_size = memory.shape[2]
    head_shape = (seqs_here, heads_here, head_size)
    query_rot = rotate(queries.astype(jnp.float32).reshape(head_shape), places)
    key_rot = rotate(keys_in.astype(jnp.float32).reshape(head_shape), places) * head_size ** (-0.5)
    value_heads = values_in.astype(jnp.float32).reshape(head_shape)
    head_index = head_first + jnp.arange(heads_here, dtype=jnp.float32)
    decays = 1.0 - jnp.exp2(-1.0 - 1.5 * head_index)
    within = jnp.sum(query_rot * key_rot, axis=-1, keepdims=True) * value_heads
    carried = (
        jnp.einsum("shd,shde->she", query_rot, memory, precision=lax.Precision.HIGHEST)
        * decays[None, :, None]
    )
    mixture = within + carried
    new_memory = (
        decays[None, :, None, None] * memory + key_rot[:, :, :, None] * value_heads[:, :, None, :]
    )
    centre = jnp.mean(mixture, axis=-1, keepdims=True)
    spread = jnp.mean(jnp.square(mixture - centre), axis=-1, keepdims=True)
    normed = ((mixture - centre) * lax.rsqrt(spread + EPSILON)).reshape(
        seqs_here, heads_here * head_size
    )
    normed = normed * head_gain.astype(jnp.float32)
    output = (jax.nn.silu(gating.astype(jnp.float32)) * normed).astype(jnp.bfloat16)
    return (output, new_memory)


def routing(routes, route_weight, capacity, slots, experts_all):
    seq_dev, top_count = routes.shape
    flat_ids = routes.reshape(-1)
    expert_ids = jnp.arange(experts_all, dtype=jnp.int32)
    onehot = (flat_ids[:, None] == expert_ids[None, :]).astype(jnp.int32)
    ranks = jnp.sum((jnp.cumsum(onehot, axis=0) - 1) * onehot, axis=1)
    slot_ids = (flat_ids * slots + ranks).reshape(seq_dev, top_count)
    slot_range = jnp.arange(experts_all * slots, dtype=jnp.int32)
    hits = slot_ids[:, :, None] == slot_range[None, None, :]
    combine = jnp.sum(
        jnp.where(hits, route_weight.astype(jnp.float32)[:, :, None], 0.0), axis=1
    ).astype(jnp.bfloat16)
    dispatch = jnp.any(slot_range[:, None, None] == slot_ids[None, :, :], axis=2)
    dispatch = dispatch.astype(jnp.bfloat16).reshape(experts_all, slots, seq_dev)
    return dispatch, combine


def tail_kernel(
    tp_count,
    ep_count,
    slots,
    part_ref,
    resid_ref,
    gain_ref,
    mix_ref,
    dispatch_ref,
    combine_ref,
    dense_gate,
    dense_up,
    dense_down,
    expert_gate,
    expert_up,
    expert_down,
    out_ref,
    wg,
    wu,
    wd,
    eg,
    eu,
    ed,
    att_rx,
    middle,
    stat_tx,
    stat_rx,
    rows,
    hot,
    tokens,
    gu_tx,
    gu_rx,
    hidden,
    eh,
    er_tx,
    er_rx,
    do_tx,
    do_rx,
    mo_tx,
    mo_rx,
    load_sem,
    send_sem,
    recv_sem,
):
    me_t = lax.axis_index("tp")
    me_e = lax.axis_index("ep")
    seq_dev, model_width = resid_ref.shape
    width = model_width // tp_count
    block = hidden.shape[0] // tp_count
    f32 = jnp.float32
    bf16 = jnp.bfloat16

    loads = [
        pltpu.make_async_copy(source, target, load_sem.at[index])
        for index, (source, target) in enumerate(
            (
                (dense_gate, wg),
                (dense_up, wu),
                (expert_gate.at[0], eg),
                (expert_up.at[0], eu),
                (expert_down.at[0], ed),
                (dense_down, wd),
            )
        )
    ]
    for load in loads:
        load.start()

    def peer_t(step):
        return lax.rem(me_t + step, tp_count)

    def peer_e(step):
        return lax.rem(me_e + step, ep_count)

    barrier = pltpu.get_barrier_semaphore()
    for step in range(1, tp_count):
        pl.semaphore_signal(
            barrier,
            inc=1,
            device_id=(me_e, peer_t(step)),
            device_id_type=pl.DeviceIdType.MESH,
        )
    for step in range(1, ep_count):
        pl.semaphore_signal(
            barrier,
            inc=1,
            device_id=(peer_e(step), me_t),
            device_id_type=pl.DeviceIdType.MESH,
        )
    pl.semaphore_wait(barrier, tp_count - 1 + ep_count - 1)

    used = [0]
    started = []

    def send(source, target, device):
        index = used[0]
        used[0] = index + 1
        copy = pltpu.make_async_remote_copy(
            src_ref=source,
            dst_ref=target,
            send_sem=send_sem.at[index],
            recv_sem=recv_sem.at[index],
            device_id=device,
            device_id_type=pl.DeviceIdType.MESH,
        )
        copy.start()
        started.append(copy)
        return copy

    def span(index, size):
        return pl.ds(pl.multiple_of(index * size, size), size)

    def dot(left, right):
        return jnp.dot(left, right, preferred_element_type=f32)

    def arrive(copies):
        for copy in copies:
            copy.wait_recv()

    tp_steps = range(1, tp_count)
    ep_steps = range(1, ep_count)
    own = span(me_t, width)

    att = [
        send(part_ref.at[:, span(peer_t(d), width)], att_rx.at[d - 1], (me_e, peer_t(d)))
        for d in tp_steps
    ]
    hots = [
        send(dispatch_ref.at[peer_e(d)], hot.at[me_e], (peer_e(d), me_t)) for d in ep_steps
    ]
    hot[me_e] = dispatch_ref[me_e]
    gain = gain_ref[:, own].astype(f32)
    mix = mix_ref[:, own].astype(f32)
    arrive(att)
    total = part_ref[:, own].astype(f32)
    for d in tp_steps:
        total = total + att_rx[d - 1].astype(f32)
    mid = resid_ref[:, own].astype(f32) + total
    middle[...] = mid
    square = jnp.sum(mid * mid, axis=-1, keepdims=True)
    mixed = jnp.sum(mid * gain * mix, axis=-1, keepdims=True)
    lane = lax.broadcasted_iota(jnp.int32, stat_tx.shape, 1)
    stat = jnp.where(lane < 64, square, mixed)
    stat_tx[...] = stat
    stats = [send(stat_tx, stat_rx.at[d - 1], (me_e, peer_t(d))) for d in tp_steps]
    arrive(stats)
    for d in tp_steps:
        stat = stat + stat_rx[d - 1]
    inverse = lax.rsqrt(stat[:, 0:1] / model_width + EPSILON)
    mixing = jax.nn.sigmoid(inverse * stat[:, 64:65])
    rows[me_e] = (middle[...] * inverse * gain).astype(bf16)

    gathered = [send(rows.at[me_e], rows.at[me_e], (peer_e(d), me_t)) for d in ep_steps]
    arrive(hots)
    arrive(gathered)
    for s in range(ep_count):
        tokens[me_t, s * slots : (s + 1) * slots, :] = dot(hot[s], rows[s]).astype(bf16)
    toks = [send(tokens.at[me_t], tokens.at[me_t], (me_e, peer_t(d))) for d in tp_steps]
    sums = []
    all_rows = rows[...].reshape(ep_count * seq_dev, width)
    for which, weight in enumerate((wg, wu)):
        loads[which].wait()
        gu_tx[which] = dot(all_rows, weight[...]).astype(bf16)
        sums += [
            send(
                gu_tx.at[which, span(peer_t(d), block), :],
                gu_rx.at[which, d - 1],
                (me_e, peer_t(d)),
            )
            for d in tp_steps
        ]
    loads[2].wait()
    loads[3].wait()
    arrive(toks)
    tile = min(256, eg.shape[1])

    def expert_tile(index, carry):
        columns = span(index, tile)
        gate = jnp.zeros((tokens.shape[1], tile), f32)
        up = jnp.zeros((tokens.shape[1], tile), f32)
        for c in range(tp_count):
            features = slice(c * width, (c + 1) * width)
            gate = gate + dot(tokens[c], eg[features, columns])
            up = up + dot(tokens[c], eu[features, columns])
        eh[:, columns] = (jax.nn.silu(gate) * up).astype(bf16)
        return carry

    lax.fori_loop(0, eg.shape[1] // tile, expert_tile, 0)

    arrive(sums)
    gate = gu_tx[0, span(me_t, block), :].astype(f32)
    up = gu_tx[1, span(me_t, block), :].astype(f32)
    for d in tp_steps:
        gate = gate + gu_rx[0, d - 1].astype(f32)
        up = up + gu_rx[1, d - 1].astype(f32)
    mine = span(me_t, block)
    hidden[mine, :] = (jax.nn.silu(gate) * up).astype(bf16)
    hids = [
        send(hidden.at[mine, :], hidden.at[mine, :], (me_e, peer_t(d))) for d in tp_steps
    ]
    loads[4].wait()
    partials = []
    for d in range(1, tp_count + 1):
        target = peer_t(d)
        er_tx[target] = dot(eh[...], ed[:, span(target, width)]).astype(bf16)
        if d < tp_count:
            partials.append(send(er_tx.at[target], er_rx.at[d - 1], (me_e, target)))
    loads[5].wait()
    arrive(hids)
    do_tx[...] = dot(hidden[...], wd[...]).astype(bf16)
    outs = [
        send(do_tx.at[span(peer_e(d), seq_dev), :], do_rx.at[d - 1], (peer_e(d), me_t))
        for d in ep_steps
    ]
    arrive(partials)
    result = er_tx[me_t].astype(f32)
    for d in tp_steps:
        result = result + er_rx[d - 1].astype(f32)
    mo_tx[...] = result.astype(bf16)
    place = span(me_e, slots)
    backs = [
        send(mo_tx.at[span(peer_e(d), slots), :], mo_rx.at[place, :], (peer_e(d), me_t))
        for d in ep_steps
    ]
    mo_rx[place, :] = mo_tx[place, :]
    arrive(outs)
    dense = do_tx[span(me_e, seq_dev), :].astype(f32)
    for d in ep_steps:
        dense = dense + do_rx[d - 1].astype(f32)
    partly = middle[...] + mixing * dense
    arrive(backs)
    out_ref[...] = (partly + dot(combine_ref[...], mo_rx[...])).astype(bf16)
    for copy in started:
        copy.wait_send()


def tail(part, resid, gain, mix, dispatch, combine, weights, tp_count, ep_count):
    seq_dev, model_width = resid.shape
    width = model_width // tp_count
    slots = dispatch.shape[1]
    batch = seq_dev * ep_count
    block = batch // tp_count
    dense_units = weights[0].shape[1]
    expert_units = weights[3].shape[2]
    items = ep_count * slots
    bf16 = jnp.bfloat16
    peers_t = tp_count - 1
    peers_e = ep_count - 1
    copies = 7 * peers_t + 4 * peers_e
    vmem = pl.BlockSpec(memory_space=pltpu.VMEM)
    anywhere = pl.BlockSpec(memory_space=pl.ANY)
    return pl.pallas_call(
        functools.partial(tail_kernel, tp_count, ep_count, slots),
        out_shape=jax.ShapeDtypeStruct((seq_dev, width), bf16),
        in_specs=[vmem] * 6 + [anywhere] * 6,
        out_specs=vmem,
        scratch_shapes=[
            pltpu.VMEM(weights[0].shape, bf16),
            pltpu.VMEM(weights[1].shape, bf16),
            pltpu.VMEM(weights[2].shape, bf16),
            pltpu.VMEM(weights[3].shape[1:], bf16),
            pltpu.VMEM(weights[4].shape[1:], bf16),
            pltpu.VMEM(weights[5].shape[1:], bf16),
            pltpu.VMEM((peers_t, seq_dev, width), bf16),
            pltpu.VMEM((seq_dev, width), jnp.float32),
            pltpu.VMEM((seq_dev, 128), jnp.float32),
            pltpu.VMEM((peers_t, seq_dev, 128), jnp.float32),
            pltpu.VMEM((ep_count, seq_dev, width), bf16),
            pltpu.VMEM((ep_count, slots, seq_dev), bf16),
            pltpu.VMEM((tp_count, items, width), bf16),
            pltpu.VMEM((2, batch, dense_units), bf16),
            pltpu.VMEM((2, peers_t, block, dense_units), bf16),
            pltpu.VMEM((batch, dense_units), bf16),
            pltpu.VMEM((items, expert_units), bf16),
            pltpu.VMEM((tp_count, items, width), bf16),
            pltpu.VMEM((peers_t, items, width), bf16),
            pltpu.VMEM((batch, width), bf16),
            pltpu.VMEM((peers_e, seq_dev, width), bf16),
            pltpu.VMEM((items, width), bf16),
            pltpu.VMEM((items, width), bf16),
            pltpu.SemaphoreType.DMA((6,)),
            pltpu.SemaphoreType.DMA((copies,)),
            pltpu.SemaphoreType.DMA((copies,)),
        ],
        compiler_params=pltpu.CompilerParams(
            collective_id=0, has_side_effects=True, vmem_limit_bytes=40 * 1024 * 1024
        ),
        name="tail",
    )(part, resid, gain, mix, dispatch, combine, *weights)


def per_device(
    resid,
    norm_gain,
    w_query,
    w_key,
    w_value,
    w_gate,
    head_gain,
    w_output,
    state,
    positions,
    ffn_gain,
    w_mix,
    dense_gate,
    dense_up,
    dense_down,
    routes,
    route_weight,
    expert_gate,
    expert_up,
    expert_down,
):
    seq_dev = resid.shape[0]
    tp_count = lax.axis_size("tp")
    ep_count = lax.axis_size("ep")
    tp_index = lax.axis_index("tp")
    normed_in = rms_norm(resid.astype(jnp.float32), norm_gain).astype(jnp.bfloat16)

    def project(weight):
        return jnp.dot(normed_in, weight, preferred_element_type=jnp.float32).astype(jnp.bfloat16)

    heads_here = state.shape[1]
    head_first = (tp_index * heads_here).astype(jnp.float32)
    retained, new_state = retain(
        project(w_query),
        project(w_key),
        project(w_value),
        project(w_gate),
        state,
        positions,
        head_first,
        head_gain,
    )
    part = jnp.dot(retained, w_output, preferred_element_type=jnp.float32).astype(jnp.bfloat16)
    top_count = routes.shape[1]
    capacity = max(2, 2 * seq_dev * top_count // ep_count)
    slots = -(-capacity // 16) * 16
    dispatch, combine = routing(routes, route_weight, capacity, slots, ep_count)
    final = tail(
        part,
        resid,
        ffn_gain[None, :],
        w_mix[None, :],
        dispatch,
        combine,
        (dense_gate, dense_up, dense_down, expert_gate, expert_up, expert_down),
        tp_count,
        ep_count,
    )
    return (final, new_state)


def solution(mesh):
    in_specs = (
        P("ep", None),
        P(),
        P(None, "tp"),
        P(None, "tp"),
        P(None, "tp"),
        P(None, "tp"),
        P("tp"),
        P("tp", None),
        P("ep", "tp", None, None),
        P("ep"),
        P(),
        P(),
        P("tp", "ep"),
        P("tp", "ep"),
        P("ep", "tp"),
        P("ep", None),
        P("ep", None),
        P("ep", None, "tp"),
        P("ep", None, "tp"),
        P("ep", "tp", None),
    )
    out_specs = (P("ep", "tp"), P("ep", "tp", None, None))
    return jax.shard_map(
        per_device, mesh=mesh, in_specs=in_specs, out_specs=out_specs, check_vma=False
    )
```

```python
import functools

import jax
import jax.numpy as jnp
from jax import lax
from jax.experimental import pallas as pl
from jax.experimental.pallas import tpu as pltpu
from jax.sharding import PartitionSpec as P

EPSILON = 1e-06
THETA = 10000.0


def rms_norm(inputs, scaling):
    square = jnp.mean(inputs * inputs, axis=-1, keepdims=True)
    return inputs * lax.rsqrt(square + EPSILON) * scaling.astype(jnp.float32)


def rotate(inputs, places):
    halfway = inputs.shape[-1] // 2
    inverse = THETA ** (-jnp.arange(halfway, dtype=jnp.float32) / halfway)
    angles = places.astype(jnp.float32)[:, None] * inverse[None, :]
    cosine = jnp.cos(angles)[:, None, :]
    sine_of = jnp.sin(angles)[:, None, :]
    former = inputs[..., :halfway]
    latter = inputs[..., halfway:]
    return jnp.concatenate(
        [former * cosine - latter * sine_of, former * sine_of + latter * cosine], axis=-1
    )


def retain(queries, keys_in, values_in, gating, memory, places, head_first, head_gain):
    seqs_here = queries.shape[0]
    heads_here = memory.shape[1]
    head_size = memory.shape[2]
    head_shape = (seqs_here, heads_here, head_size)
    query_rot = rotate(queries.astype(jnp.float32).reshape(head_shape), places)
    key_rot = rotate(keys_in.astype(jnp.float32).reshape(head_shape), places) * head_size ** (-0.5)
    value_heads = values_in.astype(jnp.float32).reshape(head_shape)
    head_index = head_first + jnp.arange(heads_here, dtype=jnp.float32)
    decays = 1.0 - jnp.exp2(-1.0 - 1.5 * head_index)
    within = jnp.sum(query_rot * key_rot, axis=-1, keepdims=True) * value_heads
    carried = (
        jnp.einsum("shd,shde->she", query_rot, memory, precision=lax.Precision.HIGHEST)
        * decays[None, :, None]
    )
    mixture = within + carried
    new_memory = (
        decays[None, :, None, None] * memory + key_rot[:, :, :, None] * value_heads[:, :, None, :]
    )
    centre = jnp.mean(mixture, axis=-1, keepdims=True)
    spread = jnp.mean(jnp.square(mixture - centre), axis=-1, keepdims=True)
    normed = ((mixture - centre) * lax.rsqrt(spread + EPSILON)).reshape(
        seqs_here, heads_here * head_size
    )
    normed = normed * head_gain.astype(jnp.float32)
    output = (jax.nn.silu(gating.astype(jnp.float32)) * normed).astype(jnp.bfloat16)
    return (output, new_memory)


def routing(routes, route_weight, capacity, slots, experts_all):
    seq_dev, top_count = routes.shape
    flat_ids = routes.reshape(-1)
    expert_ids = jnp.arange(experts_all, dtype=jnp.int32)
    onehot = (flat_ids[:, None] == expert_ids[None, :]).astype(jnp.int32)
    ranks = jnp.sum((jnp.cumsum(onehot, axis=0) - 1) * onehot, axis=1)
    slot_ids = (flat_ids * slots + ranks).reshape(seq_dev, top_count)
    slot_range = jnp.arange(experts_all * slots, dtype=jnp.int32)
    hits = slot_ids[:, :, None] == slot_range[None, None, :]
    combine = jnp.sum(
        jnp.where(hits, route_weight.astype(jnp.float32)[:, :, None], 0.0), axis=1
    ).astype(jnp.bfloat16)
    dispatch = jnp.any(slot_range[:, None, None] == slot_ids[None, :, :], axis=2)
    dispatch = dispatch.astype(jnp.bfloat16).reshape(experts_all, slots, seq_dev)
    return dispatch, combine


def tail_kernel(
    tp_count,
    ep_count,
    slots,
    part_ref,
    resid_ref,
    scale_ref,
    dispatch_ref,
    combine_ref,
    dense_gate,
    dense_up,
    dense_down,
    expert_gate,
    expert_up,
    expert_down,
    out_ref,
    wg,
    wu,
    wd,
    eg,
    eu,
    ed,
    att_rx,
    middle,
    stat_tx,
    stat_rx,
    rows,
    hot,
    tokens,
    gu_tx,
    gu_rx,
    gu_pair,
    gu_far,
    hidden,
    eh,
    er_tx,
    er_rx,
    er_pair,
    er_far,
    do_tx,
    do_rx,
    mo_tx,
    mo_rx,
    load_sem,
    send_sem,
    recv_sem,
):
    me_t = lax.axis_index("tp")
    me_e = lax.axis_index("ep")
    seq_dev, model_width = resid_ref.shape
    width = model_width // tp_count
    block = hidden.shape[0] // tp_count
    f32 = jnp.float32
    bf16 = jnp.bfloat16

    loads = [
        pltpu.make_async_copy(source, target, load_sem.at[index])
        for index, (source, target) in enumerate(
            (
                (dense_gate, wg),
                (dense_up, wu),
                (expert_gate.at[0], eg),
                (expert_up.at[0], eu),
                (expert_down.at[0], ed),
                (dense_down, wd),
            )
        )
    ]
    for load in loads:
        load.start()

    def peer_t(step):
        return lax.rem(me_t + step, tp_count)

    def peer_e(step):
        return lax.rem(me_e + step, ep_count)

    barrier = pltpu.get_barrier_semaphore()
    for step in range(1, tp_count):
        pl.semaphore_signal(
            barrier,
            inc=1,
            device_id=(me_e, peer_t(step)),
            device_id_type=pl.DeviceIdType.MESH,
        )
    for step in range(1, ep_count):
        pl.semaphore_signal(
            barrier,
            inc=1,
            device_id=(peer_e(step), me_t),
            device_id_type=pl.DeviceIdType.MESH,
        )
    pl.semaphore_wait(barrier, tp_count - 1 + ep_count - 1)

    used = [0]
    started = []

    def send(source, target, device):
        index = used[0]
        used[0] = index + 1
        copy = pltpu.make_async_remote_copy(
            src_ref=source,
            dst_ref=target,
            send_sem=send_sem.at[index],
            recv_sem=recv_sem.at[index],
            device_id=device,
            device_id_type=pl.DeviceIdType.MESH,
        )
        copy.start()
        started.append(copy)
        return copy

    def span(index, size):
        return pl.ds(pl.multiple_of(index * size, size), size)

    def dot(left, right):
        return jnp.dot(left, right, preferred_element_type=f32)

    def arrive(copies):
        for copy in copies:
            copy.wait_recv()

    half = tp_count // 2
    sibling = me_t + 1 - 2 * lax.rem(me_t, 2)

    def across(index, step):
        return lax.rem(index + 2 * step, tp_count)

    def spread(at):
        return [
            send(at(me_t), at(me_t), (me_e, target))
            for target in [sibling] + [across(me_t, k) for k in range(1, half)]
        ]

    def pass_on(copies, at):
        waiting = [copies[0]]
        for k in range(1, half):
            copies[k].wait_recv()
            origin = across(me_t, half - k)
            waiting.append(send(at(origin), at(origin), (me_e, sibling)))
        return waiting

    tp_steps = range(1, tp_count)
    ep_steps = range(1, ep_count)
    own = span(me_t, width)

    att = [
        send(part_ref.at[:, span(peer_t(d), width)], att_rx.at[d - 1], (me_e, peer_t(d)))
        for d in tp_steps
    ]
    hots = [
        send(dispatch_ref.at[peer_e(d)], hot.at[me_e], (peer_e(d), me_t)) for d in ep_steps
    ]
    hot[me_e] = dispatch_ref[me_e]
    scales = scale_ref[:, own].astype(f32)
    gain = scales[0:1, :]
    mix = scales[1:2, :]
    arrive(att)
    total = part_ref[:, own].astype(f32)
    for d in tp_steps:
        total = total + att_rx[d - 1].astype(f32)
    mid = resid_ref[:, own].astype(f32) + total
    middle[...] = mid
    square = jnp.sum(mid * mid, axis=-1, keepdims=True)
    mixed = jnp.sum(mid * gain * mix, axis=-1, keepdims=True)
    lane = lax.broadcasted_iota(jnp.int32, stat_tx.shape, 1)
    stat = jnp.where(lane < 64, square, mixed)
    stat_tx[...] = stat
    stats = [send(stat_tx, stat_rx.at[d - 1], (me_e, peer_t(d))) for d in tp_steps]
    arrive(stats)
    for d in tp_steps:
        stat = stat + stat_rx[d - 1]
    inverse = lax.rsqrt(stat[:, 0:1] / model_width + EPSILON)
    mixing = jax.nn.sigmoid(inverse * stat[:, 64:65])
    rows[me_e] = (middle[...] * inverse * gain).astype(bf16)

    gathered = [send(rows.at[me_e], rows.at[me_e], (peer_e(d), me_t)) for d in ep_steps]
    arrive(hots)
    arrive(gathered)
    for s in range(ep_count):
        tokens[me_t, s * slots : (s + 1) * slots, :] = dot(hot[s], rows[s]).astype(bf16)
    toks = spread(lambda index: tokens.at[index])
    near = []
    all_rows = rows[...].reshape(ep_count * seq_dev, width)
    for which, weight in enumerate((wg, wu)):
        loads[which].wait()
        gu_tx[which] = lax.dot_general(
            all_rows, weight[...], (((1,), (1,)), ((), ())), preferred_element_type=f32
        ).astype(bf16)
        near.append(
            [
                send(
                    gu_tx.at[which, span(across(sibling, k), block), :],
                    gu_rx.at[which, k],
                    (me_e, sibling),
                )
                for k in range(half)
            ]
        )
    toks = pass_on(toks, lambda index: tokens.at[index])
    far = []
    for which in range(2):
        arrive(near[which])
        for k in range(1, half):
            target = across(me_t, k)
            gu_pair[which, k - 1] = (
                gu_tx[which, span(target, block), :].astype(f32) + gu_rx[which, k].astype(f32)
            ).astype(bf16)
            far.append(
                send(gu_pair.at[which, k - 1], gu_far.at[which, k - 1], (me_e, target))
            )
    loads[2].wait()
    loads[3].wait()
    arrive(toks)
    tile = min(256, eg.shape[1])

    def expert_tile(index, carry):
        columns = span(index, tile)
        gate = jnp.zeros((tokens.shape[1], tile), f32)
        up = jnp.zeros((tokens.shape[1], tile), f32)
        for c in range(tp_count):
            features = slice(c * width, (c + 1) * width)
            gate = gate + dot(tokens[c], eg[features, columns])
            up = up + dot(tokens[c], eu[features, columns])
        eh[:, columns] = (jax.nn.silu(gate) * up).astype(bf16)
        return carry

    lax.fori_loop(0, eg.shape[1] // tile, expert_tile, 0)

    arrive(far)
    gate = gu_tx[0, span(me_t, block), :].astype(f32) + gu_rx[0, 0].astype(f32)
    up = gu_tx[1, span(me_t, block), :].astype(f32) + gu_rx[1, 0].astype(f32)
    for k in range(1, half):
        gate = gate + gu_far[0, k - 1].astype(f32)
        up = up + gu_far[1, k - 1].astype(f32)
    hidden[span(me_t, block), :] = (jax.nn.silu(gate) * up).astype(bf16)
    hids = spread(lambda index: hidden.at[span(index, block), :])
    loads[4].wait()
    pairs = []
    for k in range(half):
        target = across(sibling, k)
        er_tx[k] = dot(eh[...], ed[:, span(target, width)]).astype(bf16)
        pairs.append(send(er_tx.at[k], er_rx.at[k], (me_e, sibling)))
    hids = pass_on(hids, lambda index: hidden.at[span(index, block), :])
    partials = []
    for k in range(1, half):
        target = across(me_t, k)
        summed = dot(eh[...], ed[:, span(target, width)])
        arrive(pairs[k : k + 1])
        er_pair[k - 1] = (summed + er_rx[k].astype(f32)).astype(bf16)
        partials.append(send(er_pair.at[k - 1], er_far.at[k - 1], (me_e, target)))
    loads[5].wait()
    arrive(hids)
    do_tx[...] = dot(hidden[...], wd[...]).astype(bf16)
    outs = [
        send(do_tx.at[span(peer_e(d), seq_dev), :], do_rx.at[d - 1], (peer_e(d), me_t))
        for d in ep_steps
    ]
    result = dot(eh[...], ed[:, own])
    arrive(pairs[:1])
    result = result + er_rx[0].astype(f32)
    arrive(partials)
    for k in range(1, half):
        result = result + er_far[k - 1].astype(f32)
    mo_tx[...] = result.astype(bf16)
    place = span(me_e, slots)
    backs = [
        send(mo_tx.at[span(peer_e(d), slots), :], mo_rx.at[place, :], (peer_e(d), me_t))
        for d in ep_steps
    ]
    mo_rx[place, :] = mo_tx[place, :]
    arrive(outs)
    dense = do_tx[span(me_e, seq_dev), :].astype(f32)
    for d in ep_steps:
        dense = dense + do_rx[d - 1].astype(f32)
    partly = middle[...] + mixing * dense
    arrive(backs)
    out_ref[...] = (partly + dot(combine_ref[...], mo_rx[...])).astype(bf16)
    for copy in started:
        copy.wait_send()


def tail(part, resid, scale, dispatch, combine, weights, tp_count, ep_count):
    seq_dev, model_width = resid.shape
    width = model_width // tp_count
    slots = dispatch.shape[1]
    batch = seq_dev * ep_count
    block = batch // tp_count
    dense_units = weights[0].shape[0]
    half = tp_count // 2
    expert_units = weights[3].shape[2]
    items = ep_count * slots
    bf16 = jnp.bfloat16
    peers_t = tp_count - 1
    peers_e = ep_count - 1
    copies = 7 * peers_t + 4 * peers_e
    vmem = pl.BlockSpec(memory_space=pltpu.VMEM)
    anywhere = pl.BlockSpec(memory_space=pltpu.HBM)
    return pl.pallas_call(
        functools.partial(tail_kernel, tp_count, ep_count, slots),
        out_shape=jax.ShapeDtypeStruct((seq_dev, width), bf16),
        in_specs=[vmem] * 5 + [anywhere] * 6,
        out_specs=vmem,
        scratch_shapes=[
            pltpu.VMEM(weights[0].shape, bf16),
            pltpu.VMEM(weights[1].shape, bf16),
            pltpu.VMEM(weights[2].shape, bf16),
            pltpu.VMEM(weights[3].shape[1:], bf16),
            pltpu.VMEM(weights[4].shape[1:], bf16),
            pltpu.VMEM(weights[5].shape[1:], bf16),
            pltpu.VMEM((peers_t, seq_dev, width), bf16),
            pltpu.VMEM((seq_dev, width), jnp.float32),
            pltpu.VMEM((seq_dev, 128), jnp.float32),
            pltpu.VMEM((peers_t, seq_dev, 128), jnp.float32),
            pltpu.VMEM((ep_count, seq_dev, width), bf16),
            pltpu.VMEM((ep_count, slots, seq_dev), bf16),
            pltpu.VMEM((tp_count, items, width), bf16),
            pltpu.VMEM((2, batch, dense_units), bf16),
            pltpu.VMEM((2, half, block, dense_units), bf16),
            pltpu.VMEM((2, half - 1, block, dense_units), bf16),
            pltpu.VMEM((2, half - 1, block, dense_units), bf16),
            pltpu.VMEM((batch, dense_units), bf16),
            pltpu.VMEM((items, expert_units), bf16),
            pltpu.VMEM((half, items, width), bf16),
            pltpu.VMEM((half, items, width), bf16),
            pltpu.VMEM((half - 1, items, width), bf16),
            pltpu.VMEM((half - 1, items, width), bf16),
            pltpu.VMEM((batch, width), bf16),
            pltpu.VMEM((peers_e, seq_dev, width), bf16),
            pltpu.VMEM((items, width), bf16),
            pltpu.VMEM((items, width), bf16),
            pltpu.SemaphoreType.DMA((6,)),
            pltpu.SemaphoreType.DMA((copies,)),
            pltpu.SemaphoreType.DMA((copies,)),
        ],
        compiler_params=pltpu.CompilerParams(
            collective_id=0, has_side_effects=True, vmem_limit_bytes=61 * 1024 * 1024
        ),
        name="tail",
    )(part, resid, scale, dispatch, combine, *weights)


def per_device(
    resid,
    norm_gain,
    w_query,
    w_key,
    w_value,
    w_gate,
    head_gain,
    w_output,
    state,
    positions,
    ffn_gain,
    w_mix,
    dense_gate,
    dense_up,
    dense_down,
    routes,
    route_weight,
    expert_gate,
    expert_up,
    expert_down,
):
    seq_dev = resid.shape[0]
    tp_count = lax.axis_size("tp")
    ep_count = lax.axis_size("ep")
    tp_index = lax.axis_index("tp")
    normed_in = rms_norm(resid.astype(jnp.float32), norm_gain).astype(jnp.bfloat16)

    def project(weight):
        return jnp.dot(normed_in, weight, preferred_element_type=jnp.float32).astype(jnp.bfloat16)

    heads_here = state.shape[1]
    head_first = (tp_index * heads_here).astype(jnp.float32)
    retained, new_state = retain(
        project(w_query),
        project(w_key),
        project(w_value),
        project(w_gate),
        state,
        positions,
        head_first,
        head_gain,
    )
    part = jnp.dot(retained, w_output, preferred_element_type=jnp.float32).astype(jnp.bfloat16)
    top_count = routes.shape[1]
    capacity = max(2, 2 * seq_dev * top_count // ep_count)
    slots = -(-capacity // 16) * 16
    dispatch, combine = routing(routes, route_weight, capacity, slots, ep_count)
    final = tail(
        part,
        resid,
        jnp.stack([ffn_gain, w_mix]),
        dispatch,
        combine,
        (dense_gate.T, dense_up.T, dense_down, expert_gate, expert_up, expert_down),
        tp_count,
        ep_count,
    )
    return (final, new_state)


def solution(mesh):
    in_specs = (
        P("ep", None),
        P(),
        P(None, "tp"),
        P(None, "tp"),
        P(None, "tp"),
        P(None, "tp"),
        P("tp"),
        P("tp", None),
        P("ep", "tp", None, None),
        P("ep"),
        P(),
        P(),
        P("tp", "ep"),
        P("tp", "ep"),
        P("ep", "tp"),
        P("ep", None),
        P("ep", None),
        P("ep", None, "tp"),
        P("ep", None, "tp"),
        P("ep", "tp", None),
    )
    out_specs = (P("ep", "tp"), P("ep", "tp", None, None))
    return jax.shard_map(
        per_device, mesh=mesh, in_specs=in_specs, out_specs=out_specs, check_vma=False
    )
```
